512 devices in a mesh: grp: 2 (over y), fs: 32 (over z, core), tp: 8 (over x).
Axes of the slice: x: 8, y: 2, z: 16, core: 2. Of those that a mesh axis runs over, the one named last changes fastest.
The devices are a block of a 8x8x16 slice.
Arguments:
- tokens: bfloat16 [49152, 2048], P(('grp', 'fs')), parts along dimension 0, may hold values from -6 to 6
- pre_gain: float32 [2048], replicated, may hold values from 0.1 to 1.9
- up_weight: bfloat16 [2048, 8192], P('fs', 'tp'), may hold values from -0.125 to 0.125
- down_weight: bfloat16 [8192, 2048], P(('tp', 'fs')), as said below
- post_gain: float32 [2048], P('tp'), may hold values from 0.1 to 1.9
Outputs:
- mixed: bfloat16 [49152, 2048], P(('grp', 'fs'), 'tp'), parts along dimension 0
The draws below stay inside these ranges and needn't reach their ends.
There are 2 independent parts, one for each index of `grp`. The reference program is written for one: setup_inputs(seed, part) draws one part's arguments, and reference() takes and returns one part's arrays. A program takes and returns all parts, laid end to end along the dimension named above; an argument that names none is the same for every part. Nothing has to cross between parts.
Inputs may be any that keep to these rules, and one draw needn't show every extreme that they name: `down_weight`: a matrix whose columns fall into 8 consecutive blocks of different magnitudes.
All inputs are finite; a program needn't handle non-finite values.
Results may differ from the reference program's by a relative error of at most 0.014.
Values may be sent and summed in bfloat16 or wider, within the bound.
No kernel may reach another device: no remote copies, remote signals or barrier semaphores. Data moves between devices by JAX's collectives and lax.ppermute only.
A program may use at most 64 MiB of HBM per device.

```python
import jax
import jax.numpy as jnp
from jax import lax

D = 2048
FF = 8192
TOKENS = 24576
N_TP = 8


def draw_down_weight(key, part):
    first, second = jax.random.split(key, 2)
    levels = jnp.exp(jnp.linspace(jnp.log(0.3), jnp.log(3.0), N_TP)).astype(jnp.float32)
    order = jax.random.permutation(first, N_TP)
    levels = levels[order]
    column_block = jnp.arange(D) // (D // N_TP)
    column_scale = levels[column_block]
    base = jax.random.normal(second, (FF, D), jnp.float32)
    return (base * column_scale[None, :] * FF ** (-0.5)).astype(jnp.bfloat16)


def shard_levels(own_key, dims, shards, low, top_value):
    gain = 1.0
    for axis_at, parts in shards:
        steps = jax.random.uniform(jax.random.fold_in(jax.random.fold_in(own_key, 6), axis_at), (parts,), jnp.float32, low / len(shards), top_value / len(shards))
        gain = gain * jnp.repeat(jnp.exp(steps), dims[axis_at] // parts).reshape((-1,) + (1,) * (len(dims) - 1 - axis_at))
    return gain


def bell_draw(key, extent, scale, bound, shards=(), held_as=jnp.bfloat16):
    entries = jax.random.normal(key, extent, jnp.float32) * scale
    if len(shards) > 0:
        entries = shard_levels(key, extent, shards, -0.22, 0.18) * entries
    return jnp.clip(entries, min=-bound, max=bound).astype(held_as)


def setup_inputs(seed: int = 0, part: int = 0) -> dict:
    key_of = jax.random.split(jax.random.key(seed), 6)
    part_keys = jax.random.split(jax.random.fold_in(key_of[5], part), 6)
    tokens = bell_draw(part_keys[0], (TOKENS, D), 1.0, 6.0, ((0, 32),))
    pre_gain = jnp.clip(1.0 + 0.18 * jax.random.normal(key_of[1], (D,), jnp.float32), 0.1, 1.9)
    up_weight = bell_draw(key_of[2], (D, FF), D ** -0.5, 0.125, ((0, 32), (1, 8)))
    down_weight = draw_down_weight(jax.random.fold_in(key_of[5], 71), part)
    post_gain = jnp.clip(1.0 + 0.18 * jax.random.normal(key_of[4], (D,), jnp.float32), 0.1, 1.9)
    return {"tokens": tokens, "pre_gain": pre_gain, "up_weight": up_weight, "down_weight": down_weight, "post_gain": post_gain}


def reference(tokens, pre_gain, up_weight, down_weight, post_gain):
    eps = 1e-06
    values = tokens.astype(jnp.float32)
    normed = (values * lax.rsqrt(lax.optimization_barrier(jnp.mean(values * values, axis=1, keepdims=True)) + eps) * pre_gain).astype(jnp.bfloat16)
    block = FF // N_TP
    total = jnp.zeros((tokens.shape[0], D), jnp.float32)
    for index in range(N_TP):
        up = jnp.dot(normed, up_weight[:, index * block:(index + 1) * block], preferred_element_type=jnp.float32)
        hidden = jnp.square(jnp.maximum(up, 0.0)).astype(jnp.bfloat16)
        part = jnp.dot(hidden, down_weight[index * block:(index + 1) * block, :], preferred_element_type=jnp.float32).astype(jnp.bfloat16)
        part = lax.optimization_barrier(part)
        total = total + part.astype(jnp.float32)
    factor = lax.rsqrt(lax.optimization_barrier(jnp.mean(total * total, axis=1, keepdims=True)) + eps)
    return (total * factor * post_gain).astype(jnp.bfloat16)
```

```python
import functools

import jax
import jax.numpy as jnp
from jax import lax
from jax.experimental import pallas as pl
from jax.experimental.pallas import tpu as pltpu
from jax.sharding import PartitionSpec as P


def from_everyone(value, axis):
    copies = jnp.broadcast_to(value, (lax.axis_size(axis), *value.shape))
    return lax.all_to_all(copies, axis, split_axis=0, concat_axis=0, tiled=True)


def of_everyone(value, axis):
    everything = from_everyone(value, axis)
    return jnp.sum(everything, axis=0)


def norm_kernel(x_ref, gain_ref, out_ref):
    x = x_ref[...].astype(jnp.float32)
    factor = lax.rsqrt(jnp.mean(x * x, axis=1, keepdims=True) + 1e-6)
    out_ref[...] = (x * factor * gain_ref[...]).astype(jnp.bfloat16)


def norm(tokens, gain, rows):
    count, width = tokens.shape
    return pl.pallas_call(
        norm_kernel,
        grid=(count // rows,),
        in_specs=[
            pl.BlockSpec((rows, width), lambda i: (i, 0)),
            pl.BlockSpec((1, width), lambda i: (0, 0)),
        ],
        out_specs=pl.BlockSpec((rows, width), lambda i: (i, 0)),
        out_shape=jax.ShapeDtypeStruct((count, width), jnp.bfloat16),
        name="pre_norm",
    )(tokens, gain.reshape(1, width))


def layer_kernel(packed, x_ref, out_ref, up_v, down_v, hidden_v, up_sem, down_sem, *, shards, up_rows, down_rows):
    step = pl.program_id(0)
    width = up_v.shape[1]
    cols = out_ref.shape[1]
    parts = down_v.shape[1] // width
    rows = up_rows + parts * down_rows

    def up_copy(s):
        return pltpu.make_async_copy(
            packed.at[pl.ds(s * rows, up_rows)], up_v.at[pl.ds(s * up_rows, up_rows)], up_sem.at[s]
        )

    def down_copy(s, p):
        return pltpu.make_async_copy(
            packed.at[pl.ds(s * rows + up_rows + p * down_rows, down_rows)],
            down_v.at[pl.ds(s * down_rows, down_rows), pl.ds(p * width, width)],
            down_sem.at[p * shards + s],
        )

    @pl.when(step == 0)
    def _():
        def start_up(s, c):
            up_copy(s).start()
            return c

        lax.fori_loop(0, shards, start_up, 0)
        for p in range(parts):
            def start_down(s, c, p=p):
                down_copy(s, p).start()
                return c

            lax.fori_loop(0, shards, start_down, 0)

        def wait_up(s, c):
            up_copy(s).wait()
            return c

        lax.fori_loop(0, shards, wait_up, 0)
        piece = 512
        for n in range(width // piece):
            span = slice(n * piece, (n + 1) * piece)
            up = jnp.dot(x_ref[...], up_v[:, span], preferred_element_type=jnp.float32)
            hidden_v[:, span] = jnp.square(jnp.maximum(up, 0.0)).astype(jnp.bfloat16)

        for p in range(parts):
            def wait_down(s, c, p=p):
                down_copy(s, p).wait()
                return c

            lax.fori_loop(0, shards, wait_down, 0)

    start = pl.multiple_of(step * cols, cols)
    out_ref[...] = jnp.dot(
        hidden_v[...], down_v[:, pl.ds(start, cols)], preferred_element_type=jnp.float32
    ).astype(jnp.bfloat16)


def layer(packed, normed, shards, up_rows, down_rows):
    count, width = normed.shape
    hidden = packed.shape[1]
    cols = 512
    return pl.pallas_call(
        functools.partial(layer_kernel, shards=shards, up_rows=up_rows, down_rows=down_rows),
        grid=(width // cols,),
        in_specs=[
            pl.BlockSpec(memory_space=pl.ANY),
            pl.BlockSpec((count, width), lambda j: (0, 0)),
        ],
        out_specs=pl.BlockSpec((count, cols), lambda j: (0, j)),
        out_shape=jax.ShapeDtypeStruct((count, width), jnp.bfloat16),
        scratch_shapes=[
            pltpu.VMEM((width, hidden), jnp.bfloat16),
            pltpu.VMEM((hidden, width), jnp.bfloat16),
            pltpu.VMEM((count, hidden), jnp.bfloat16),
            pltpu.SemaphoreType.DMA((shards,)),
            pltpu.SemaphoreType.DMA((shards * (width // hidden),)),
        ],
        compiler_params=pltpu.CompilerParams(vmem_limit_bytes=40 * 1024 * 1024),
        name="layer",
    )(packed, normed)


def shards(tokens, pre_gain, up_weight, down_weight, post_gain):
    eps = 1e-06
    fs = lax.axis_size("fs")
    hidden = up_weight.shape[1]
    width = down_weight.shape[1]
    pieces = [up_weight] + [down_weight[:, p * hidden:(p + 1) * hidden] for p in range(width // hidden)]
    packed = lax.all_gather(jnp.concatenate(pieces, axis=0), "fs", axis=0, tiled=True)
    normed = norm(tokens, pre_gain, 256)
    partial_terms = layer(packed, normed, fs, up_weight.shape[0], down_weight.shape[0])
    own_width = post_gain.shape[0]
    full_width = lax.axis_size("tp") * own_width
    mixed = lax.psum_scatter(partial_terms, "tp", scatter_dimension=1, tiled=True).astype(jnp.float32)
    squares = of_everyone(jnp.sum(mixed * mixed, axis=1), "tp")
    factor = lax.rsqrt(squares / full_width + eps)
    return (mixed * factor[:, None] * post_gain).astype(jnp.bfloat16)


def solution(mesh):
    in_specs = (P(("grp", "fs"), None), P(), P("fs", "tp"), P(("tp", "fs"), None), P("tp"))
    out_specs = P(("grp", "fs"), "tp")
    return jax.shard_map(shards, mesh=mesh, in_specs=in_specs, out_specs=out_specs, check_vma=False)
```

```python
import functools

import jax
import jax.numpy as jnp
from jax import lax
from jax.experimental import pallas as pl
from jax.experimental.pallas import tpu as pltpu
from jax.sharding import PartitionSpec as P

LANES = 1024
TOP = 2.0 ** 15
UP_FACTORS = 3
DOWN_FACTORS = 5


def from_everyone(value, axis):
    copies = jnp.broadcast_to(value, (lax.axis_size(axis), *value.shape))
    return lax.all_to_all(copies, axis, split_axis=0, concat_axis=0, tiled=True)


def of_everyone(value, axis):
    everything = from_everyone(value, axis)
    return jnp.sum(everything, axis=0)


def power_factors(top, count):
    factors = []
    for _ in range(count):
        factor = jnp.ones_like(top)
        for power in (8, 4, 2):
            factor = jnp.where(top * factor * 2.0**power <= TOP, factor * 2.0**power, factor)
        for power in (8, 4, 2):
            factor = jnp.where(top * factor > TOP * 2.0 ** (power - 2), factor * 2.0**-power, factor)
        top = top * factor
        factors.append(factor)
    return factors


def largest(value):
    return jnp.max(jnp.max(jnp.abs(value), axis=0, keepdims=True), axis=1, keepdims=True)


def pack_kernel(order_ref, up_ref, down_ref, out_ref, *, own):
    up_rows = up_ref.shape[0]
    down_rows = down_ref.shape[0]
    up = up_ref[...].astype(jnp.float32)
    up_factors = power_factors(jnp.broadcast_to(largest(up), (1, LANES)), UP_FACTORS)
    for factor in up_factors:
        up = up * factor
    out_ref[0:up_rows, :] = up.astype(jnp.bfloat16)
    top = largest(down_ref[...].astype(jnp.float32))
    down_factors = power_factors(jnp.broadcast_to(top, (1, LANES)), DOWN_FACTORS)
    for j in range(down_ref.shape[1] // own):
        start = pl.multiple_of(order_ref[j] * own, own)
        piece = down_ref[:, pl.ds(start, own)].astype(jnp.float32)
        for factor in down_factors:
            piece = piece * factor[:, :own]
        row = up_rows + down_rows * (j * own // LANES)
        column = j * own % LANES
        out_ref[row:row + down_rows, column:column + own] = piece.astype(jnp.bfloat16)
    row = up_rows + down_rows * (down_ref.shape[1] // LANES)
    inverses = [1.0 / factor for factor in up_factors + down_factors]
    out_ref[row:, :] = jnp.concatenate(inverses, axis=0).astype(jnp.bfloat16)


def pack(order, up_weight, down_weight, own):
    rows = up_weight.shape[0] + down_weight.shape[0] * (down_weight.shape[1] // LANES)
    return pl.pallas_call(
        functools.partial(pack_kernel, own=own),
        in_specs=[
            pl.BlockSpec(memory_space=pltpu.SMEM),
            pl.BlockSpec(memory_space=pltpu.VMEM),
            pl.BlockSpec(memory_space=pltpu.VMEM),
        ],
        out_shape=jax.ShapeDtypeStruct((rows + UP_FACTORS + DOWN_FACTORS, LANES), jnp.bfloat16),
        name="pack",
    )(order, up_weight, down_weight)


def first_kernel(x_ref, gain_ref, up_ref, inverse_ref, down_ref, hidden_ref, part_ref, up_scale, down_scale):
    shards = inverse_ref.shape[0]

    @pl.when(pl.program_id(0) == 0)
    def _():
        for scale, first, count in ((up_scale, 0, UP_FACTORS), (down_scale, UP_FACTORS, DOWN_FACTORS)):
            width = scale.shape[1]
            per = width // shards
            for p in range(width // LANES):
                owner = (lax.broadcasted_iota(jnp.int32, (1, LANES), 1) + p * LANES) // per
                total = jnp.zeros((1, LANES), jnp.float32)
                for s in range(p * LANES // per, ((p + 1) * LANES - 1) // per + 1):
                    rows = inverse_ref[s].astype(jnp.float32)
                    value = rows[first:first + 1]
                    for t in range(1, count):
                        value = value * rows[first + t:first + t + 1]
                    value = jnp.concatenate([value] * (LANES // value.shape[1]), axis=1)
                    total = jnp.where(owner == s, value, total)
                scale[:, p * LANES:(p + 1) * LANES] = total

    x = x_ref[...].astype(jnp.float32)
    factor = lax.rsqrt(jnp.mean(x * x, axis=1, keepdims=True) + 1e-6)
    normed = (x * factor * gain_ref[...]).astype(jnp.bfloat16) * up_scale[...].astype(jnp.bfloat16)
    up = jnp.dot(normed, up_ref[...], preferred_element_type=jnp.float32)
    hidden = (jnp.square(jnp.maximum(up, 0.0)) * down_scale[...]).astype(jnp.bfloat16)
    hidden_ref[...] = hidden
    part_ref[...] = jnp.dot(hidden, down_ref[...], preferred_element_type=jnp.float32).astype(jnp.bfloat16)


def first(tokens, gain, up, inverses, down, start, rows):
    width = tokens.shape[1]
    hidden = up.shape[1]
    own = down.shape[1]
    whole = lambda *shape: pl.BlockSpec(shape, lambda i: (0,) * len(shape))
    return pl.pallas_call(
        first_kernel,
        grid=(1,),
        in_specs=[
            pl.BlockSpec((rows, width), lambda i: (start, 0)),
            whole(1, width),
            whole(*up.shape),
            whole(*inverses.shape),
            whole(*down.shape),
        ],
        out_specs=[whole(rows, hidden), whole(rows, own)],
        out_shape=[
            jax.ShapeDtypeStruct((rows, hidden), jnp.bfloat16),
            jax.ShapeDtypeStruct((rows, own), jnp.bfloat16),
        ],
        scratch_shapes=[pltpu.VMEM((1, width), jnp.float32), pltpu.VMEM((1, hidden), jnp.float32)],
        compiler_params=pltpu.CompilerParams(vmem_limit_bytes=24 * 1024 * 1024),
        name="first",
    )(tokens, gain.reshape(1, width), up, inverses, down)


def rest_kernel(top_ref, bottom_ref, down_ref, out_ref):
    half = top_ref.shape[0]
    own = out_ref.shape[2]
    for j in range(out_ref.shape[0]):
        down = down_ref[:, j * own:(j + 1) * own]
        for at, hidden_ref in ((0, top_ref), (half, bottom_ref)):
            part = jnp.dot(hidden_ref[...], down, preferred_element_type=jnp.float32)
            out_ref[j, at:at + half, :] = part.astype(jnp.bfloat16)


def rest(top, bottom, down, own):
    return pl.pallas_call(
        rest_kernel,
        out_shape=jax.ShapeDtypeStruct((down.shape[1] // own, 2 * top.shape[0], own), jnp.bfloat16),
        compiler_params=pltpu.CompilerParams(vmem_limit_bytes=16 * 1024 * 1024),
        name="rest",
    )(top, bottom, down)


def add(a, b):
    return (a.astype(jnp.float32) + b.astype(jnp.float32)).astype(jnp.bfloat16)


def shards(tokens, pre_gain, up_weight, down_weight, post_gain):
    eps = 1e-06
    fs = lax.axis_size("fs")
    tp = lax.axis_size("tp")
    me = lax.axis_index("tp")
    up_rows, down_rows = up_weight.shape[0], down_weight.shape[0]
    own = post_gain.shape[0]
    half = tokens.shape[0] // 2
    offsets = [tp // 2]
    for distance in range(tp // 2 - 1, 0, -1):
        offsets += [distance, tp - distance]
    offsets.append(0)
    order = (me + jnp.array(offsets, jnp.int32)) % tp
    packed = pack(order, up_weight, down_weight, own)
    rows = packed.shape[0]
    scales = UP_FACTORS + DOWN_FACTORS
    everything = lax.all_gather(packed.astype(jnp.float16), "fs", axis=0, tiled=False)

    def down(source, start, stop):
        pieces = []
        while start < stop:
            column = start * own % LANES
            width = min((stop - start) * own, LANES - column)
            row = up_rows + down_rows * (start * own // LANES)
            piece = source[:, row:row + down_rows, column:column + width].astype(jnp.bfloat16)
            pieces.append(piece.reshape(fs * down_rows, width))
            start += width // own
        return pieces

    up = everything[:, :up_rows].astype(jnp.bfloat16).reshape(fs * up_rows, LANES)
    inverses = everything[:, rows - scales:, :128].astype(jnp.bfloat16)
    far_down, = down(everything, 0, 1)
    top, top_part = first(tokens, pre_gain, up, inverses, far_down, 0, half)
    bottom, bottom_part = first(tokens, pre_gain, up, inverses, far_down, 1, half)

    right = [(i, (i + 1) % tp) for i in range(tp)]
    left = [(i, (i - 1) % tp) for i in range(tp)]
    from_left = lax.ppermute(top_part, "tp", right)
    from_right = lax.ppermute(bottom_part, "tp", left)
    held, bottom = lax.optimization_barrier((everything, bottom))
    parts = []
    for piece in down(held, 1, 3):
        got = rest(top, bottom, piece, own)
        parts += [got[j] for j in range(got.shape[0])]
    for step in range(tp // 2 - 1):
        to_right, to_left = parts[2 * step], parts[2 * step + 1]
        if step == 0:
            to_right = jnp.concatenate([add(from_left, to_right[:half]), to_right[half:]], axis=0)
            to_left = jnp.concatenate([to_left[:half], add(from_right, to_left[half:])], axis=0)
        else:
            to_right = add(from_left, to_right)
            to_left = add(from_right, to_left)
        from_left = lax.ppermute(to_right, "tp", right)
        from_right = lax.ppermute(to_left, "tp", left)
        if step == 0:
            held, to_right = lax.optimization_barrier((held, to_right))
            for piece in down(held, 3, tp):
                got = rest(top, bottom, piece, own)
                parts += [got[j] for j in range(got.shape[0])]
    mixed = parts[-1].astype(jnp.float32) + from_left.astype(jnp.float32) + from_right.astype(jnp.float32)
    squares = of_everyone(jnp.sum(mixed * mixed, axis=1), "tp")
    factor = lax.rsqrt(squares / (tp * own) + eps)
    return (mixed * factor[:, None] * post_gain).astype(jnp.bfloat16)


def solution(mesh):
    in_specs = (P(("grp", "fs"), None), P(), P("fs", "tp"), P(("tp", "fs"), None), P("tp"))
    out_specs = P(("grp", "fs"), "tp")
    return jax.shard_map(shards, mesh=mesh, in_specs=in_specs, out_specs=out_specs, check_vma=False)
```

```python
import functools

import jax
import jax.numpy as jnp
from jax import lax
from jax.experimental import pallas as pl
from jax.experimental.pallas import tpu as pltpu
from jax.sharding import PartitionSpec as P

TOP = 2.0 ** 15
UP_FACTORS = 3
DOWN_FACTORS = 5


def from_everyone(value, axis):
    copies = jnp.broadcast_to(value, (lax.axis_size(axis), *value.shape))
    return lax.all_to_all(copies, axis, split_axis=0, concat_axis=0, tiled=True)


def of_everyone(value, axis):
    everything = from_everyone(value, axis)
    return jnp.sum(everything, axis=0)


def power_factors(top, count):
    factors = []
    for _ in range(count):
        factor = jnp.ones_like(top)
        for power in (8, 4, 2):
            factor = jnp.where(top * factor * 2.0**power <= TOP, factor * 2.0**power, factor)
        for power in (8, 4, 2):
            factor = jnp.where(top * factor > TOP * 2.0 ** (power - 2), factor * 2.0**-power, factor)
        top = top * factor
        factors.append(factor)
    return factors


def largest(value):
    return jnp.max(jnp.max(jnp.abs(value), axis=0, keepdims=True), axis=1, keepdims=True)


def pack_kernel(up_hbm, down_hbm, out_ref, up_ref, down_ref, sems, *, offsets):
    fetches = [
        pltpu.make_async_copy(source, target, sems.at[i])
        for i, (source, target) in enumerate(((up_hbm, up_ref), (down_hbm, down_ref)))
    ]
    for fetch in fetches:
        fetch.start()
    own = out_ref.shape[1]
    up_rows = up_ref.shape[0]
    down_rows = down_ref.shape[0]
    fetches[0].wait()
    up = up_ref[...].astype(jnp.float32)
    up_factors = power_factors(jnp.broadcast_to(largest(up), (1, own)), UP_FACTORS)
    at = 0
    for j in range(up_ref.shape[1] // own):
        piece = up[:, j * own:(j + 1) * own]
        for factor in up_factors:
            piece = piece * factor
        out_ref[at:at + up_rows, :] = piece.astype(jnp.bfloat16)
        at += up_rows
    fetches[1].wait()
    top = largest(down_ref[...].astype(jnp.float32))
    down_factors = power_factors(jnp.broadcast_to(top, (1, own)), DOWN_FACTORS)
    for offset in offsets:
        start = pl.multiple_of((lax.axis_index("tp") + offset) % len(offsets) * own, own)
        piece = down_ref[:, pl.ds(start, own)].astype(jnp.float32)
        for factor in down_factors:
            piece = piece * factor
        out_ref[at:at + down_rows, :] = piece.astype(jnp.bfloat16)
        at += down_rows
    inverses = [1.0 / factor for factor in up_factors + down_factors]
    out_ref[at:, :] = jnp.concatenate(inverses, axis=0).astype(jnp.bfloat16)


def pack(up_weight, down_weight, own, offsets):
    rows = (up_weight.size + down_weight.size) // own + UP_FACTORS + DOWN_FACTORS
    hbm = pl.BlockSpec(memory_space=pltpu.HBM)
    return pl.pallas_call(
        functools.partial(pack_kernel, offsets=offsets),
        in_specs=[hbm, hbm],
        out_shape=jax.ShapeDtypeStruct((rows, own), jnp.bfloat16),
        scratch_shapes=[
            pltpu.VMEM(up_weight.shape, jnp.bfloat16),
            pltpu.VMEM(down_weight.shape, jnp.bfloat16),
            pltpu.SemaphoreType.DMA((2,)),
        ],
        compiler_params=pltpu.CompilerParams(vmem_limit_bytes=8 * 1024 * 1024),
        name="pack",
    )(up_weight, down_weight)


def first_kernel(x_ref, gain_ref, up_ref, inverse_ref, down_ref, hidden_ref, part_ref, up_scale, down_scale):
    shards, _, own = inverse_ref.shape
    up_rows = x_ref.shape[1] // shards

    @pl.when(pl.program_id(0) == 0)
    def _():
        for scale, first, count in ((up_scale, 0, UP_FACTORS), (down_scale, UP_FACTORS, DOWN_FACTORS)):
            per = scale.shape[1] // shards
            for p in range(scale.shape[1] // own):
                owner = (lax.broadcasted_iota(jnp.int32, (1, own), 1) + p * own) // per
                total = jnp.zeros((1, own), jnp.float32)
                for s in range(p * own // per, ((p + 1) * own - 1) // per + 1):
                    rows = inverse_ref[s].astype(jnp.float32)
                    value = rows[first:first + 1]
                    for t in range(1, count):
                        value = value * rows[first + t:first + t + 1]
                    total = jnp.where(owner == s, value, total)
                scale[:, p * own:(p + 1) * own] = total

    x = x_ref[...].astype(jnp.float32)
    factor = lax.rsqrt(jnp.mean(x * x, axis=1, keepdims=True) + 1e-6)
    normed = (x * factor * gain_ref[...]).astype(jnp.bfloat16) * up_scale[...].astype(jnp.bfloat16)
    for q in range(hidden_ref.shape[1] // own):
        weights = up_ref[:, q * up_rows:(q + 1) * up_rows, :].reshape(x_ref.shape[1], own)
        span = slice(q * own, (q + 1) * own)
        up = jnp.dot(normed, weights, preferred_element_type=jnp.float32)
        hidden_ref[:, span] = (jnp.square(jnp.maximum(up, 0.0)) * down_scale[:, span]).astype(jnp.bfloat16)
    down = down_ref[...].reshape(hidden_ref.shape[1], own)
    part_ref[...] = jnp.dot(hidden_ref[...], down, preferred_element_type=jnp.float32).astype(jnp.bfloat16)


def first(tokens, gain, up, inverses, down, rows):
    count, width = tokens.shape
    shards, _, own = down.shape
    hidden = shards * down.shape[1]
    whole = lambda *shape: pl.BlockSpec(shape, lambda i: (0,) * len(shape))
    return pl.pallas_call(
        first_kernel,
        grid=(count // rows,),
        in_specs=[
            pl.BlockSpec((rows, width), lambda i: (i, 0)),
            whole(1, width),
            whole(*up.shape),
            whole(*inverses.shape),
            whole(*down.shape),
        ],
        out_specs=[pl.BlockSpec((rows, hidden), lambda i: (i, 0)), pl.BlockSpec((rows, own), lambda i: (i, 0))],
        out_shape=[
            jax.ShapeDtypeStruct((count, hidden), jnp.bfloat16),
            jax.ShapeDtypeStruct((count, own), jnp.bfloat16),
        ],
        scratch_shapes=[pltpu.VMEM((1, width), jnp.float32), pltpu.VMEM((1, hidden), jnp.float32)],
        compiler_params=pltpu.CompilerParams(vmem_limit_bytes=20 * 1024 * 1024),
        name="first",
    )(tokens, gain.reshape(1, width), up, inverses, down)


def rest_kernel(hidden_ref, down_ref, *out_refs):
    width = hidden_ref.shape[1]
    rows = width // down_ref.shape[0]
    for j, out_ref in enumerate(out_refs):
        own = out_ref.shape[1]
        paired = j < len(out_refs) // 2 * 2
        block = (j + lax.axis_index("fs")) % 2 + j // 2 * 2 if paired else j
        start = pl.multiple_of(block * rows, rows)
        down = down_ref[:, pl.ds(start, rows), :].reshape(width, own)
        out_ref[...] = jnp.dot(hidden_ref[...], down, preferred_element_type=jnp.float32).astype(jnp.bfloat16)


def rest(hidden, down):
    shards, rows, own = down.shape
    count = rows // (hidden.shape[1] // shards)
    vmem = pl.BlockSpec(memory_space=pltpu.VMEM)
    return pl.pallas_call(
        rest_kernel,
        in_specs=[vmem, vmem],
        out_specs=[vmem] * count,
        out_shape=[jax.ShapeDtypeStruct((hidden.shape[0], own), jnp.bfloat16)] * count,
        compiler_params=pltpu.CompilerParams(vmem_limit_bytes=8 * 1024 * 1024),
        name="rest",
    )(hidden, down)


def add(a, b):
    return (a.astype(jnp.float32) + b.astype(jnp.float32)).astype(jnp.bfloat16)


def shards(tokens, pre_gain, up_weight, down_weight, post_gain):
    eps = 1e-06
    fs = lax.axis_size("fs")
    tp = lax.axis_size("tp")
    own = post_gain.shape[0]
    up_rows = up_weight.size // own
    down_rows = down_weight.shape[0]
    offsets = [tp // 2]
    for distance in range(tp // 2 - 1, 0, -1):
        offsets += [distance, tp - distance]
    offsets.append(0)
    packed = pack(up_weight, down_weight, own, offsets)
    everything = lax.all_gather(packed.astype(jnp.float16), "fs", axis=0, tiled=False)

    def down(source, start, stop):
        return source[:, up_rows + start * down_rows:up_rows + stop * down_rows].astype(jnp.bfloat16)

    up = everything[:, :up_rows].astype(jnp.bfloat16)
    inverses = everything[:, up_rows + tp * down_rows:].astype(jnp.bfloat16)
    hidden, one = first(tokens, pre_gain, up, inverses, down(everything, 0, 1), tokens.shape[0] // 2)

    def send(value, sign):
        pairs = []
        for f in range(fs):
            step = sign if f % 2 == 0 else -sign
            pairs += [(f * tp + t, f * tp + (t + step) % tp) for t in range(tp)]
        return lax.ppermute(value, ("fs", "tp"), pairs)

    one = send(one, 1)
    held, hidden = lax.optimization_barrier((everything, hidden))
    *parts, own_part = rest(hidden, down(held, 1, tp))
    two = send(parts[1], -1)
    one = send(add(one, parts[0]), 1)
    for step in range(1, tp // 2 - 1):
        two = send(add(two, parts[2 * step + 1]), -1)
        one = send(add(one, parts[2 * step]), 1)
    mixed = own_part.astype(jnp.float32) + one.astype(jnp.float32) + two.astype(jnp.float32)
    squares = of_everyone(jnp.sum(mixed * mixed, axis=1), "tp")
    factor = lax.rsqrt(squares / (tp * own) + eps)
    return (mixed * factor[:, None] * post_gain).astype(jnp.bfloat16)


def solution(mesh):
    in_specs = (P(("grp", "fs"), None), P(), P("fs", "tp"), P(("tp", "fs"), None), P("tp"))
    out_specs = P(("grp", "fs"), "tp")
    return jax.shard_map(shards, mesh=mesh, in_specs=in_specs, out_specs=out_specs, check_vma=False)
```

```python
import functools

import jax
import jax.numpy as jnp
from jax import lax
from jax.experimental import pallas as pl
from jax.experimental.pallas import tpu as pltpu
from jax.sharding import PartitionSpec as P

TOP = 2.0 ** 15
UP_FACTORS = 3
DOWN_FACTORS = 5


def from_everyone(value, axis):
    copies = jnp.broadcast_to(value, (lax.axis_size(axis), *value.shape))
    return lax.all_to_all(copies, axis, split_axis=0, concat_axis=0, tiled=True)


def of_everyone(value, axis):
    everything = from_everyone(value, axis)
    return jnp.sum(everything, axis=0)


def power_factors(top, count):
    factors = []
    for _ in range(count):
        factor = jnp.ones_like(top)
        for power in (8, 4, 2):
            factor = jnp.where(top * factor * 2.0**power <= TOP, factor * 2.0**power, factor)
        for power in (8, 4, 2):
            factor = jnp.where(top * factor > TOP * 2.0 ** (power - 2), factor * 2.0**-power, factor)
        top = top * factor
        factors.append(factor)
    return factors


def largest(value):
    return jnp.max(jnp.max(jnp.abs(value), axis=0, keepdims=True), axis=1, keepdims=True)


def pack_kernel(up_hbm, down_hbm, out_ref, up_ref, down_ref, sems, *, offsets):
    fetches = [
        pltpu.make_async_copy(source, target, sems.at[i])
        for i, (source, target) in enumerate(((up_hbm, up_ref), (down_hbm, down_ref)))
    ]
    for fetch in fetches:
        fetch.start()
    own = out_ref.shape[1]
    up_rows = up_ref.shape[0]
    down_rows = down_ref.shape[0]
    fetches[0].wait()
    up = up_ref[...].astype(jnp.float32)
    up_factors = power_factors(jnp.broadcast_to(largest(up), (1, own)), UP_FACTORS)
    at = 0
    for j in range(up_ref.shape[1] // own):
        piece = up[:, j * own:(j + 1) * own]
        for factor in up_factors:
            piece = piece * factor
        out_ref[at:at + up_rows, :] = piece.astype(jnp.bfloat16)
        at += up_rows
    fetches[1].wait()
    top = largest(down_ref[...].astype(jnp.float32))
    down_factors = power_factors(jnp.broadcast_to(top, (1, own)), DOWN_FACTORS)
    for offset in offsets:
        start = pl.multiple_of((lax.axis_index("tp") + offset) % len(offsets) * own, own)
        piece = down_ref[:, pl.ds(start, own)].astype(jnp.float32)
        for factor in down_factors:
            piece = piece * factor
        out_ref[at:at + down_rows, :] = piece.astype(jnp.bfloat16)
        at += down_rows
    inverses = [1.0 / factor for factor in up_factors + down_factors]
    out_ref[at:, :] = jnp.concatenate(inverses, axis=0).astype(jnp.bfloat16)


def pack(up_weight, down_weight, own, offsets):
    rows = (up_weight.size + down_weight.size) // own + UP_FACTORS + DOWN_FACTORS
    hbm = pl.BlockSpec(memory_space=pltpu.HBM)
    return pl.pallas_call(
        functools.partial(pack_kernel, offsets=offsets),
        in_specs=[hbm, hbm],
        out_shape=jax.ShapeDtypeStruct((rows, own), jnp.bfloat16),
        scratch_shapes=[
            pltpu.VMEM(up_weight.shape, jnp.bfloat16),
            pltpu.VMEM(down_weight.shape, jnp.bfloat16),
            pltpu.SemaphoreType.DMA((2,)),
        ],
        compiler_params=pltpu.CompilerParams(vmem_limit_bytes=8 * 1024 * 1024),
        name="pack",
    )(up_weight, down_weight)


def first_kernel(x_ref, gain_ref, up_ref, inverse_ref, down_ref, hidden_ref, one_ref, two_ref, up_scale, down_scale):
    shards, _, own = inverse_ref.shape
    up_rows = x_ref.shape[1] // shards

    @pl.when(pl.program_id(0) == 0)
    def _():
        for scale, first, count in ((up_scale, 0, UP_FACTORS), (down_scale, UP_FACTORS, DOWN_FACTORS)):
            per = scale.shape[1] // shards
            for p in range(scale.shape[1] // own):
                owner = (lax.broadcasted_iota(jnp.int32, (1, own), 1) + p * own) // per
                total = jnp.zeros((1, own), jnp.float32)
                for s in range(p * own // per, ((p + 1) * own - 1) // per + 1):
                    rows = inverse_ref[s].astype(jnp.float32)
                    value = rows[first:first + 1]
                    for t in range(1, count):
                        value = value * rows[first + t:first + t + 1]
                    total = jnp.where(owner == s, value, total)
                scale[:, p * own:(p + 1) * own] = total

    x = x_ref[...].astype(jnp.float32)
    factor = lax.rsqrt(jnp.mean(x * x, axis=1, keepdims=True) + 1e-6)
    normed = (x * factor * gain_ref[...]).astype(jnp.bfloat16) * up_scale[...].astype(jnp.bfloat16)
    for q in range(hidden_ref.shape[1] // own):
        weights = up_ref[:, q * up_rows:(q + 1) * up_rows, :].reshape(x_ref.shape[1], own)
        span = slice(q * own, (q + 1) * own)
        up = jnp.dot(normed, weights, preferred_element_type=jnp.float32)
        hidden_ref[:, span] = (jnp.square(jnp.maximum(up, 0.0)) * down_scale[:, span]).astype(jnp.bfloat16)
    down_rows = hidden_ref.shape[1] // shards
    for j, part_ref in enumerate((one_ref, two_ref)):
        down = down_ref[:, j * down_rows:(j + 1) * down_rows, :].reshape(hidden_ref.shape[1], own)
        part_ref[...] = jnp.dot(hidden_ref[...], down, preferred_element_type=jnp.float32).astype(jnp.bfloat16)


def first(tokens, gain, up, inverses, down, rows):
    count, width = tokens.shape
    shards, _, own = down.shape
    hidden = shards * down.shape[1] // 2
    whole = lambda *shape: pl.BlockSpec(shape, lambda i: (0,) * len(shape))
    return pl.pallas_call(
        first_kernel,
        grid=(count // rows,),
        in_specs=[
            pl.BlockSpec((rows, width), lambda i: (i, 0)),
            whole(1, width),
            whole(*up.shape),
            whole(*inverses.shape),
            whole(*down.shape),
        ],
        out_specs=[pl.BlockSpec((rows, columns), lambda i: (i, 0)) for columns in (hidden, own, own)],
        out_shape=[jax.ShapeDtypeStruct((count, columns), jnp.bfloat16) for columns in (hidden, own, own)],
        scratch_shapes=[pltpu.VMEM((1, width), jnp.float32), pltpu.VMEM((1, hidden), jnp.float32)],
        compiler_params=pltpu.CompilerParams(vmem_limit_bytes=20 * 1024 * 1024),
        name="first",
    )(tokens, gain.reshape(1, width), up, inverses, down)


def rest_kernel(hidden_ref, down_ref, *refs, blocks, turn):
    width = hidden_ref.shape[1]
    rows = width // down_ref.shape[0]
    mine = lax.axis_index("fs") % 2 == turn

    @pl.when(mine)
    def _():
        for j, out_ref in enumerate(refs[-blocks:]):
            down = down_ref[:, j * rows:(j + 1) * rows, :].reshape(width, out_ref.shape[1])
            part = jnp.dot(hidden_ref[...], down, preferred_element_type=jnp.float32)
            out_ref[...] = part.astype(jnp.bfloat16)

    if len(refs) > blocks:
        @pl.when(jnp.logical_not(mine))
        def _():
            for held_ref, out_ref in zip(refs[:blocks], refs[blocks:]):
                out_ref[...] = held_ref[...]


def rest(hidden, down, parts, turn):
    shards, rows, own = down.shape
    count = rows // (hidden.shape[1] // shards)
    vmem = pl.BlockSpec(memory_space=pltpu.VMEM)
    return pl.pallas_call(
        functools.partial(rest_kernel, blocks=count, turn=turn),
        in_specs=[vmem] * (2 + len(parts)),
        out_specs=[vmem] * count,
        out_shape=[jax.ShapeDtypeStruct((hidden.shape[0], own), jnp.bfloat16)] * count,
        compiler_params=pltpu.CompilerParams(vmem_limit_bytes=8 * 1024 * 1024),
        name="rest",
    )(hidden, down, *parts)


def add(a, b):
    return (a.astype(jnp.float32) + b.astype(jnp.float32)).astype(jnp.bfloat16)


def shards(tokens, pre_gain, up_weight, down_weight, post_gain):
    eps = 1e-06
    fs = lax.axis_size("fs")
    tp = lax.axis_size("tp")
    own = post_gain.shape[0]
    up_rows = up_weight.size // own
    down_rows = down_weight.shape[0]
    offsets = [tp // 2, tp // 2 + 1, tp // 2 - 1]
    for distance in range(tp // 2 - 2, 0, -1):
        offsets += [distance, tp - distance]
    offsets.append(0)
    packed = pack(up_weight, down_weight, own, offsets)
    everything = lax.all_gather(packed.astype(jnp.float16), "fs", axis=0, tiled=False)

    def down(source, start, stop):
        return source[:, up_rows + start * down_rows:up_rows + stop * down_rows].astype(jnp.bfloat16)

    up = everything[:, :up_rows].astype(jnp.bfloat16)
    inverses = everything[:, up_rows + tp * down_rows:].astype(jnp.bfloat16)
    hidden, one, two = first(tokens, pre_gain, up, inverses, down(everything, 0, 2), tokens.shape[0] // 2)

    def send(value, step):
        return lax.ppermute(value, "tp", [(t, (t + step) % tp) for t in range(tp)])

    held, hidden = lax.optimization_barrier((everything, hidden))
    rest_down = down(held, 2, tp)
    parts = rest(hidden, rest_down, [], 0)
    one, two, *parts = lax.optimization_barrier((one, two, *parts))
    one = send(one, 1)
    two = send(two, -1)
    part_one, *parts, own_part = rest(hidden, rest_down, parts, 1)
    one = send(add(one, part_one), 1)
    for step in range(tp // 2 - 2):
        two = send(add(two, parts[2 * step + 1]), -1)
        one = send(add(one, parts[2 * step]), 1)
    mixed = own_part.astype(jnp.float32) + one.astype(jnp.float32) + two.astype(jnp.float32)
    squares = of_everyone(jnp.sum(mixed * mixed, axis=1), "tp")
    factor = lax.rsqrt(squares / (tp * own) + eps)
    return (mixed * factor[:, None] * post_gain).astype(jnp.bfloat16)


def solution(mesh):
    in_specs = (P(("grp", "fs"), None), P(), P("fs", "tp"), P(("tp", "fs"), None), P("tp"))
    out_specs = P(("grp", "fs"), "tp")
    return jax.shard_map(shards, mesh=mesh, in_specs=in_specs, out_specs=out_specs, check_vma=False)
```

```python
import functools

import jax
import jax.numpy as jnp
from jax import lax
from jax.experimental import pallas as pl
from jax.experimental.pallas import tpu as pltpu
from jax.sharding import PartitionSpec as P

TOP = 2.0 ** 15
UP_FACTORS = 3
DOWN_FACTORS = 5


def from_everyone(value, axis):
    copies = jnp.broadcast_to(value, (lax.axis_size(axis), *value.shape))
    return lax.all_to_all(copies, axis, split_axis=0, concat_axis=0, tiled=True)


def of_everyone(value, axis):
    everything = from_everyone(value, axis)
    return jnp.sum(everything, axis=0)


def power_factors(top, count):
    factors = []
    for _ in range(count):
        factor = jnp.ones_like(top)
        for power in (8, 4, 2):
            factor = jnp.where(top * factor * 2.0**power <= TOP, factor * 2.0**power, factor)
        for power in (8, 4, 2):
            factor = jnp.where(top * factor > TOP * 2.0 ** (power - 2), factor * 2.0**-power, factor)
        top = top * factor
        factors.append(factor)
    return factors


def largest(value):
    return jnp.max(jnp.max(jnp.abs(value), axis=0, keepdims=True), axis=1, keepdims=True)


def pack_kernel(up_hbm, down_hbm, out_ref, up_ref, down_ref, sems, *, offsets):
    fetches = [
        pltpu.make_async_copy(source, target, sems.at[i])
        for i, (source, target) in enumerate(((up_hbm, up_ref), (down_hbm, down_ref)))
    ]
    for fetch in fetches:
        fetch.start()
    own = out_ref.shape[1]
    up_rows = up_ref.shape[0]
    down_rows = down_ref.shape[0]
    fetches[0].wait()
    up = up_ref[...].astype(jnp.float32)
    up_factors = power_factors(jnp.broadcast_to(largest(up), (1, own)), UP_FACTORS)
    at = 0
    for j in range(up_ref.shape[1] // own):
        piece = up[:, j * own:(j + 1) * own]
        for factor in up_factors:
            piece = piece * factor
        out_ref[at:at + up_rows, :] = piece.astype(jnp.bfloat16)
        at += up_rows
    fetches[1].wait()
    top = largest(down_ref[...].astype(jnp.float32))
    down_factors = power_factors(jnp.broadcast_to(top, (1, own)), DOWN_FACTORS)
    for offset in offsets:
        start = pl.multiple_of((lax.axis_index("tp") + offset) % len(offsets) * own, own)
        piece = down_ref[:, pl.ds(start, own)].astype(jnp.float32)
        for factor in down_factors:
            piece = piece * factor
        out_ref[at:at + down_rows, :] = piece.astype(jnp.bfloat16)
        at += down_rows
    inverses = [1.0 / factor for factor in up_factors + down_factors]
    out_ref[at:, :] = jnp.concatenate(inverses, axis=0).astype(jnp.bfloat16)


def pack(up_weight, down_weight, own, offsets):
    rows = (up_weight.size + down_weight.size) // own + UP_FACTORS + DOWN_FACTORS
    hbm = pl.BlockSpec(memory_space=pltpu.HBM)
    return pl.pallas_call(
        functools.partial(pack_kernel, offsets=offsets),
        in_specs=[hbm, hbm],
        out_shape=jax.ShapeDtypeStruct((rows, own), jnp.bfloat16),
        scratch_shapes=[
            pltpu.VMEM(up_weight.shape, jnp.bfloat16),
            pltpu.VMEM(down_weight.shape, jnp.bfloat16),
            pltpu.SemaphoreType.DMA((2,)),
        ],
        compiler_params=pltpu.CompilerParams(vmem_limit_bytes=8 * 1024 * 1024),
        name="pack",
    )(up_weight, down_weight)


def first_kernel(x_ref, gain_ref, up_ref, inverse_ref, down_ref, hidden_ref, one_ref, two_ref, up_scale, down_scale):
    shards, _, own = inverse_ref.shape
    up_rows = x_ref.shape[1] // shards

    @pl.when(pl.program_id(0) == 0)
    def _():
        for scale, first, count in ((up_scale, 0, UP_FACTORS), (down_scale, UP_FACTORS, DOWN_FACTORS)):
            per = scale.shape[1] // shards
            for p in range(scale.shape[1] // own):
                owner = (lax.broadcasted_iota(jnp.int32, (1, own), 1) + p * own) // per
                total = jnp.zeros((1, own), jnp.float32)
                for s in range(p * own // per, ((p + 1) * own - 1) // per + 1):
                    rows = inverse_ref[s].astype(jnp.float32)
                    value = rows[first:first + 1]
                    for t in range(1, count):
                        value = value * rows[first + t:first + t + 1]
                    total = jnp.where(owner == s, value, total)
                scale[:, p * own:(p + 1) * own] = total

    x = x_ref[...].astype(jnp.float32)
    factor = lax.rsqrt(jnp.mean(x * x, axis=1, keepdims=True) + 1e-6)
    normed = (x * factor * gain_ref[...]).astype(jnp.bfloat16) * up_scale[...].astype(jnp.bfloat16)
    for q in range(hidden_ref.shape[1] // own):
        weights = up_ref[:, q * up_rows:(q + 1) * up_rows, :].reshape(x_ref.shape[1], own)
        span = slice(q * own, (q + 1) * own)
        up = jnp.dot(normed, weights, preferred_element_type=jnp.float32)
        hidden_ref[:, span] = (jnp.square(jnp.maximum(up, 0.0)) * down_scale[:, span]).astype(jnp.bfloat16)
    down_rows = hidden_ref.shape[1] // shards
    for j, part_ref in enumerate((one_ref, two_ref)):
        down = down_ref[:, j * down_rows:(j + 1) * down_rows, :].reshape(hidden_ref.shape[1], own)
        part_ref[...] = jnp.dot(hidden_ref[...], down, preferred_element_type=jnp.float32).astype(jnp.bfloat16)


def first(tokens, gain, up, inverses, down, rows):
    count, width = tokens.shape
    shards, _, own = down.shape
    hidden = shards * down.shape[1] // 2
    whole = lambda *shape: pl.BlockSpec(shape, lambda i: (0,) * len(shape))
    return pl.pallas_call(
        first_kernel,
        grid=(count // rows,),
        in_specs=[
            pl.BlockSpec((rows, width), lambda i: (i, 0)),
            whole(1, width),
            whole(*up.shape),
            whole(*inverses.shape),
            whole(*down.shape),
        ],
        out_specs=[pl.BlockSpec((rows, columns), lambda i: (i, 0)) for columns in (hidden, own, own)],
        out_shape=[jax.ShapeDtypeStruct((count, columns), jnp.bfloat16) for columns in (hidden, own, own)],
        scratch_shapes=[pltpu.VMEM((1, width), jnp.float32), pltpu.VMEM((1, hidden), jnp.float32)],
        compiler_params=pltpu.CompilerParams(vmem_limit_bytes=20 * 1024 * 1024),
        name="first",
    )(tokens, gain.reshape(1, width), up, inverses, down)


def rest_kernel(hidden_ref, down_ref, *refs, blocks, turn):
    width = hidden_ref.shape[1]
    rows = width // down_ref.shape[0]
    mine = lax.axis_index("fs") % 2 == turn

    @pl.when(mine)
    def _():
        for j, out_ref in enumerate(refs[-blocks:]):
            down = down_ref[:, j * rows:(j + 1) * rows, :].reshape(width, out_ref.shape[1])
            part = jnp.dot(hidden_ref[...], down, preferred_element_type=jnp.float32)
            out_ref[...] = part.astype(jnp.bfloat16)

    if len(refs) > blocks:
        @pl.when(jnp.logical_not(mine))
        def _():
            for held_ref, out_ref in zip(refs[:blocks], refs[blocks:]):
                out_ref[...] = held_ref[...]


def rest(hidden, down, parts, turn):
    shards, rows, own = down.shape
    count = rows // (hidden.shape[1] // shards)
    vmem = pl.BlockSpec(memory_space=pltpu.VMEM)
    return pl.pallas_call(
        functools.partial(rest_kernel, blocks=count, turn=turn),
        in_specs=[vmem] * (2 + len(parts)),
        out_specs=[vmem] * count,
        out_shape=[jax.ShapeDtypeStruct((hidden.shape[0], own), jnp.bfloat16)] * count,
        compiler_params=pltpu.CompilerParams(vmem_limit_bytes=8 * 1024 * 1024),
        name="rest",
    )(hidden, down, *parts)


def add(a, b):
    return (a.astype(jnp.float32) + b.astype(jnp.float32)).astype(jnp.bfloat16)


def shards(tokens, pre_gain, up_weight, down_weight, post_gain):
    eps = 1e-06
    fs = lax.axis_size("fs")
    tp = lax.axis_size("tp")
    own = post_gain.shape[0]
    up_rows = up_weight.size // own
    down_rows = down_weight.shape[0]
    offsets = [tp // 2, tp // 2 - 1, tp // 2 + 1]
    for distance in range(tp // 2 - 2, 0, -1):
        offsets += [tp - distance, distance]
    offsets.append(0)
    packed = pack(up_weight, down_weight, own, offsets)
    everything = lax.all_gather(packed.astype(jnp.float16), "fs", axis=0, tiled=False)

    def down(source, start, stop):
        return source[:, up_rows + start * down_rows:up_rows + stop * down_rows].astype(jnp.bfloat16)

    up = everything[:, :up_rows].astype(jnp.bfloat16)
    inverses = everything[:, up_rows + tp * down_rows:].astype(jnp.bfloat16)
    hidden, one, two = first(tokens, pre_gain, up, inverses, down(everything, 0, 2), tokens.shape[0] // 2)

    def send(value, step):
        return lax.ppermute(value, "tp", [(t, (t + step) % tp) for t in range(tp)])

    held, hidden = lax.optimization_barrier((everything, hidden))
    rest_down = down(held, 2, tp)
    parts = rest(hidden, rest_down, [], 0)
    one, two, *parts = lax.optimization_barrier((one, two, *parts))
    one = send(one, -1)
    two = send(two, 1)
    part_one, *parts, own_part = rest(hidden, rest_down, parts, 1)
    one = send(add(one, part_one), -1)
    for step in range(tp // 2 - 2):
        two = send(add(two, parts[2 * step + 1]), 1)
        one = send(add(one, parts[2 * step]), -1)
    mixed = own_part.astype(jnp.float32) + one.astype(jnp.float32) + two.astype(jnp.float32)
    squares = of_everyone(jnp.sum(mixed * mixed, axis=1), "tp")
    factor = lax.rsqrt(squares / (tp * own) + eps)
    return (mixed * factor[:, None] * post_gain).astype(jnp.bfloat16)


def solution(mesh):
    in_specs = (P(("grp", "fs"), None), P(), P("fs", "tp"), P(("tp", "fs"), None), P("tp"))
    out_specs = P(("grp", "fs"), "tp")
    return jax.shard_map(shards, mesh=mesh, in_specs=in_specs, out_specs=out_specs, check_vma=False)
```
